32 devices in a mesh: ep: 8 (over z, x), tp: 4 (over y, core).
Axes of the slice: x: 2, y: 2, z: 4, core: 2. Of those that a mesh axis runs over, the one named last changes fastest.
Arguments:
- mixer_query: bfloat16 [2048, 2048], P('ep', 'tp'), may hold values from -6 to 6
- mixer_forget: bfloat16 [2048, 2048], P('ep', 'tp'), may hold values from -5.5 to 5.5
- mixer_value: bfloat16 [2048, 2048], P('ep', 'tp'), may hold values from -6 to 6
- mixer_gate: bfloat16 [2048, 2048], P('ep', 'tp'), may hold values from -6 to 6
- forget_floor: float32 [2048], P('tp'), may hold values from 0.88 to 1
- head_gain: float32 [128], replicated, may hold values from 0.1 to 1.9
- mixer_proj: bfloat16 [2048, 2048], P(None, 'tp'), may hold values from -0.125 to 0.125
- expert_tokens: bfloat16 [1024, 2048], P('ep'), may hold values from -6 to 6
- expert_gain: float32 [2048], replicated, may hold values from 0.1 to 1.9
- routes: int32 [1024, 2], P('ep'), may hold values from 0 to 7, as said below
- group_logits: float32 [1024, 4], P('ep'), may hold values from -6 to 6
- choice_logits: float32 [1024, 2], P('ep'), may hold values from -6 to 6
- w_gate: bfloat16 [8, 2048, 2048], P('ep', None, 'tp'), may hold values from -0.125 to 0.125
- w_up: bfloat16 [8, 2048, 2048], P('ep', None, 'tp'), may hold values from -0.125 to 0.125
- w_down: bfloat16 [8, 2048, 2048], P('ep', None, 'tp'), may hold values from -0.125 to 0.125
Outputs:
- mixer_out: bfloat16 [2048, 2048], P('ep', 'tp')
- expert_out: bfloat16 [1024, 2048], P('ep', 'tp')
The draws below stay inside these ranges and needn't reach their ends.
Inputs may be any that keep to these rules, and one draw needn't show every extreme that they name: `routes`: in each aligned block of 128 rows (the rows of one index of ep) no expert is named by more than 64 rows, and some expert reaches that bound in every block; the 2 experts of a row differ and lie in the same group.
All inputs are finite; a program needn't handle non-finite values.
Results may differ from the reference program's by a relative error of at most 0.01.
Values may be sent and summed in bfloat16 or wider, within the bound.
A program may use at most 64 MiB of HBM per device.

```python
import math
import jax
import jax.numpy as jnp
from jax import lax

D = 2048
HEADS = 16
KEYDIM = 128
VDIM = 128
FF = 2048
GROUPS = 4
TOPK = 2
BLOCK = 64
TOKA_DEV = 256
TOKB_DEV = 128
EXPERTS = 8
EXP_GROUP = 2
CAP = 64
TOKENS_A = 2048
TOKENS_B = 1024
N_EP = 8


def draw_mixer_forget(key, part):
    noise_key = jax.random.fold_in(key, 11)
    shift_key = jax.random.fold_in(key, 12)
    noise = jnp.clip(jax.random.normal(noise_key, (TOKENS_A, HEADS * KEYDIM), jnp.float32), -4.0, 4.0)
    shifts = jax.random.uniform(shift_key, (TOKENS_A // TOKA_DEV, 1, 1), jnp.float32, -1.5, 1.5)
    shaped = noise.reshape(TOKENS_A // TOKA_DEV, TOKA_DEV, HEADS * KEYDIM) + shifts
    return shaped.reshape(TOKENS_A, HEADS * KEYDIM).astype(jnp.bfloat16)


def draw_forget_floor(key, part):
    pick_key = jax.random.fold_in(key, 21)
    slow_key = jax.random.fold_in(key, 22)
    fast_key = jax.random.fold_in(key, 23)
    slow_share = 0.5
    slow_heads = jax.random.uniform(pick_key, (HEADS, 1), jnp.float32) < slow_share
    slow_gap = jax.random.uniform(slow_key, (HEADS, KEYDIM), jnp.float32, 0.3, 2.0) / TOKENS_A
    fast_gap = jnp.exp(jax.random.uniform(fast_key, (HEADS, KEYDIM), jnp.float32, math.log(0.03), math.log(0.12)))
    gap_rows = jnp.where(slow_heads, slow_gap, fast_gap)
    return (1.0 - gap_rows).reshape(HEADS * KEYDIM).astype(jnp.float32)


def route_block(block_key):
    group_size = EXPERTS // GROUPS
    quota = TOKB_DEV // EXPERTS
    expert_ids = jnp.arange(EXPERTS, dtype=jnp.int32)
    counts = jnp.full((EXPERTS,), quota, jnp.int32)
    counts = counts + quota * ((expert_ids == 0) | (expert_ids == group_size - 1)).astype(jnp.int32)
    counts = counts - quota * ((expert_ids == group_size) | (expert_ids == group_size + 1)).astype(jnp.int32)
    canonical = jnp.repeat(expert_ids, counts, total_repeat_length=TOKB_DEV)
    order = jax.random.permutation(jax.random.fold_in(block_key, 1), TOKB_DEV)
    first = canonical[order]
    second = first // group_size * group_size + (first % group_size + 1) % group_size
    group_map = jax.random.permutation(jax.random.fold_in(block_key, 2), GROUPS).astype(jnp.int32)
    rotation = jax.random.randint(jax.random.fold_in(block_key, 3), (GROUPS,), 0, group_size).astype(jnp.int32)

    def relabel(ids):
        grp = ids // group_size
        return (group_map[grp] * group_size + (ids % group_size + rotation[grp]) % group_size).astype(jnp.int32)
    first = relabel(first)
    second = relabel(second)
    flip = jax.random.randint(jax.random.fold_in(block_key, 4), (TOKB_DEV,), 0, 2).astype(jnp.int32)
    left = flip * second + (1 - flip) * first
    right = flip * first + (1 - flip) * second
    return jnp.stack([left, right], axis=-1).astype(jnp.int32)


def draw_routes(key, part):
    base_key = jax.random.fold_in(key, 31)
    block_keys = jax.vmap(lambda index: jax.random.fold_in(base_key, index))(jnp.arange(N_EP))
    return jax.vmap(route_block)(block_keys).reshape(TOKENS_B, TOPK).astype(jnp.int32)


def steps_of(key, extent, cuts, least, largest):
    gain, own = 1.0, jax.random.fold_in(key, 6)
    for position, blocks in cuts:
        steps = jnp.exp(jax.random.uniform(jax.random.fold_in(own, position), (blocks,), jnp.float32, least / len(cuts), largest / len(cuts)))
        gain = gain * jnp.repeat(steps, extent[position] // blocks).reshape([-1 if axis == position else 1 for axis in range(len(extent))])
    return gain


def bell_draw(rng, shape, scale, bound, cuts=(), kind=jnp.bfloat16):
    loudness = steps_of(rng, shape, cuts, -0.22, 0.18) if cuts else 1.0
    values = jax.random.normal(rng, shape, jnp.float32) * scale * loudness
    return jnp.minimum(jnp.maximum(values, -bound), bound).astype(kind)


def setup_inputs(seed: int = 0) -> dict:
    key_of = jax.random.split(jax.random.key(seed), 16)
    return {
        "mixer_query": bell_draw(key_of[0], (TOKENS_A, HEADS * KEYDIM), 1.0, 6.0, ((0, 8), (1, 4))),
        "mixer_forget": draw_mixer_forget(jax.random.fold_in(key_of[15], 71), 0),
        "mixer_value": bell_draw(key_of[2], (TOKENS_A, HEADS * VDIM), 1.0, 6.0, ((0, 8), (1, 4))),
        "mixer_gate": bell_draw(key_of[3], (TOKENS_A, HEADS * VDIM), 1.0, 6.0, ((0, 8), (1, 4))),
        "forget_floor": draw_forget_floor(jax.random.fold_in(key_of[15], 71), 0),
        "head_gain": jnp.clip(1.0 + 0.18 * jax.random.normal(key_of[5], (VDIM,), jnp.float32), 0.1, 1.9),
        "mixer_proj": bell_draw(key_of[6], (HEADS * VDIM, D), (HEADS * VDIM) ** -0.5, 0.125, ((1, 4),)),
        "expert_tokens": bell_draw(key_of[7], (TOKENS_B, D), 1.0, 6.0, ((0, 8),)),
        "expert_gain": jnp.clip(1.0 + 0.18 * jax.random.normal(key_of[8], (D,), jnp.float32), 0.1, 1.9),
        "routes": draw_routes(jax.random.fold_in(key_of[15], 71), 0),
        "group_logits": bell_draw(key_of[10], (TOKENS_B, GROUPS), 1.0, 6.0, ((0, 8),), jnp.float32),
        "choice_logits": bell_draw(key_of[11], (TOKENS_B, TOPK), 1.0, 6.0, ((0, 8),), jnp.float32),
        "w_gate": bell_draw(key_of[12], (EXPERTS, D, FF), D ** -0.5, 0.125, ((0, 8), (2, 4))),
        "w_up": bell_draw(key_of[13], (EXPERTS, D, FF), D ** -0.5, 0.125, ((0, 8), (2, 4))),
        "w_down": bell_draw(key_of[14], (EXPERTS, FF, D), FF ** -0.5, 0.125, ((0, 8), (2, 4))),
    }


norm_eps = 1e-06
highest_precision = lax.Precision.HIGHEST

def rms_scale(features, gain_vec):
    return features * lax.rsqrt(lax.optimization_barrier(jnp.mean(features * features, axis=-1, keepdims=True)) + norm_eps) * gain_vec

def block_terms(query_block, input_block, log_blk, value_block, carried_state):
    cumulative_log = jnp.cumsum(log_blk, axis=0)
    between_block_term = jnp.einsum('zug,ugr->zur', query_block * jnp.exp(cumulative_log), carried_state, precision=highest_precision)
    causal = jnp.tril(jnp.ones((query_block.shape[0], query_block.shape[0]), dtype=bool))[:, :, None, None]
    differ = cumulative_log[:, None] - cumulative_log[None, :]
    decays = jnp.exp(jnp.where(causal, differ, -jnp.inf))
    scores = lax.optimization_barrier(jnp.sum(query_block[:, None] * input_block[None, :] * decays, axis=-1))
    result = between_block_term + jnp.einsum('tsh,shv->thv', scores, value_block, precision=highest_precision)
    ending_log_decay = cumulative_log[-1]
    updated_state = jnp.exp(ending_log_decay)[..., None] * carried_state + jnp.einsum('twa,twr->war', input_block * jnp.exp(ending_log_decay[None] - cumulative_log), value_block, precision=highest_precision)
    return (updated_state, result, cumulative_log)

def mixer_part(mixer_query, mixer_forget, mixer_value, mixer_gate, forget_floor, head_gain, mixer_proj):
    length = mixer_query.shape[0]
    blocks = length // BLOCK

    def split_blocks(source_array, last_width):
        return source_array.reshape(blocks, BLOCK, HEADS, last_width)
    queries = jax.nn.silu(mixer_query.astype(jnp.float32))
    input_rates = (1.0 - forget_floor) * jax.nn.sigmoid(-mixer_forget.astype(jnp.float32))
    log_forget = jnp.log1p(-input_rates)
    value_rows = mixer_value.astype(jnp.float32)

    def advance(carried_state, block_inputs):
        query_block, input_block, value_block, log_blk = block_inputs
        updated_state, result, cumulative_log = block_terms(query_block, input_block, log_blk, value_block, carried_state)
        return (updated_state, result)
    initial = jnp.zeros((HEADS, KEYDIM, VDIM), jnp.float32)
    _, output_rows = lax.scan(advance, initial, (split_blocks(queries, KEYDIM), split_blocks(input_rates, KEYDIM), split_blocks(value_rows, VDIM), split_blocks(log_forget, KEYDIM)))
    output_rows = output_rows.reshape(length, HEADS, VDIM)
    gate_act = jax.nn.silu(mixer_gate.astype(jnp.float32)).reshape(length, HEADS, VDIM)
    gated_out = rms_scale(output_rows, head_gain) * gate_act
    mixed_heads = gated_out.reshape(length, HEADS * VDIM).astype(jnp.bfloat16)
    return jnp.dot(mixed_heads, mixer_proj, preferred_element_type=jnp.float32).astype(jnp.bfloat16)

def gate_weights(routes, group_logits, choice_logits, group_size):
    group_exp = jnp.exp(group_logits)
    group_prob = group_exp / lax.optimization_barrier(jnp.sum(group_exp, axis=-1, keepdims=True))
    groups_of = routes // group_size
    member = (groups_of[..., None] == jnp.arange(GROUPS, dtype=jnp.int32)).astype(jnp.float32)
    picked_prob = lax.optimization_barrier(jnp.sum(member * group_prob[:, None, :], axis=-1))
    choice_exp = jnp.exp(choice_logits)
    together = (groups_of[:, :, None] == groups_of[:, None, :]).astype(jnp.float32)
    within = lax.optimization_barrier(jnp.sum(together * choice_exp[:, None, :], axis=-1))
    return picked_prob * choice_exp / within

def rank_slots(flat_routes, per_block, expert_count):
    onehot = (flat_routes[:, None] == jnp.arange(expert_count, dtype=jnp.int32)).astype(jnp.int32)
    blocked = onehot.reshape(-1, per_block, expert_count)
    earlier = (jnp.cumsum(blocked, axis=1) - blocked).astype(jnp.int32)
    return lax.optimization_barrier(jnp.sum(earlier * blocked, axis=-1)).astype(jnp.int32).reshape(-1)

def expert_part(expert_tokens, expert_gain, routes, group_logits, choice_logits, w_gate, w_up, w_down):
    count_rows = expert_tokens.shape[0]
    normed = rms_scale(expert_tokens.astype(jnp.float32), expert_gain).astype(jnp.bfloat16)
    weights = gate_weights(routes, group_logits, choice_logits, EXP_GROUP)
    flat_routes = routes.reshape(-1)
    per_block = TOKB_DEV * TOPK
    ranks = rank_slots(flat_routes, per_block, EXPERTS)
    block_ids = (jnp.arange(flat_routes.shape[0], dtype=jnp.int32) // per_block).astype(jnp.int32)
    slot_of = (flat_routes * (N_EP * CAP) + block_ids * CAP + ranks).astype(jnp.int32)
    token_ids = (jnp.arange(flat_routes.shape[0], dtype=jnp.int32) // TOPK).astype(jnp.int32)
    token_of = jnp.full((EXPERTS * N_EP * CAP,), count_rows, jnp.int32).at[slot_of].set(token_ids)
    padded = jnp.concatenate([normed, jnp.zeros((1, D), jnp.bfloat16)], axis=0)

    def run_expert(operands):
        gate_mat, up_mat, down_mat, index_rows = operands
        chosen = padded[index_rows]
        gate_pre = jnp.dot(chosen, gate_mat, preferred_element_type=jnp.float32)
        up_pre = jnp.dot(chosen, up_mat, preferred_element_type=jnp.float32)
        hidden = (jax.nn.silu(gate_pre) * up_pre).astype(jnp.bfloat16)
        return jnp.dot(hidden, down_mat, preferred_element_type=jnp.float32).astype(jnp.bfloat16)
    output_rows = lax.map(run_expert, (w_gate, w_up, w_down, token_of.reshape(EXPERTS, N_EP * CAP)))
    picked = output_rows.reshape(-1, D)[slot_of].astype(jnp.float32) * weights.reshape(-1)[:, None]
    return lax.optimization_barrier(jnp.sum(picked.reshape(count_rows, TOPK, D), axis=1)).astype(jnp.bfloat16)

def reference(mixer_query, mixer_forget, mixer_value, mixer_gate, forget_floor, head_gain, mixer_proj, expert_tokens, expert_gain, routes, group_logits, choice_logits, w_gate, w_up, w_down):
    mixer_out = mixer_part(mixer_query, mixer_forget, mixer_value, mixer_gate, forget_floor, head_gain, mixer_proj)
    expert_out = expert_part(expert_tokens, expert_gain, routes, group_logits, choice_logits, w_gate, w_up, w_down)
    return (mixer_out, expert_out)
```

```python
import functools

import jax
import jax.numpy as jnp
from jax import lax
from jax.experimental import pallas as pl
from jax.experimental.pallas import tpu as pltpu
from jax.sharding import PartitionSpec as P

KEYDIM = 128
GROUPS = 4
TOPK = 2
CORES = 2
BATCHES = 2
norm_eps = 1e-06
MESH = pl.DeviceIdType.MESH
f32 = jnp.float32
bf16 = jnp.bfloat16


def mm(a, b):
    return jnp.dot(a, b, preferred_element_type=f32)


def mm_nt(a, b):
    return lax.dot_general(a, b, (((1,), (1,)), ((), ())), preferred_element_type=f32)


def mm_tn(a, b):
    return lax.dot_general(a, b, (((0,), (0,)), ((), ())), preferred_element_type=f32)


def sigmoid(v):
    return 1.0 / (1.0 + jnp.exp(-v))


class Gather:
    def __init__(self, buf, width, tall, ranks, sems):
        self.buf, self.width, self.tall = buf, width, tall
        self.t, self.m = ranks
        self.y, self.c, self.ys = self.t // CORES, self.t % CORES, self.m // CORES
        self.ds, self.dr, self.ps, self.pr = sems
        self.sent = []

    def place(self, y, c, k):
        t = y * CORES + c
        cols = pl.ds(pl.multiple_of(t * self.width, self.width), self.width)
        return self.buf.at[pl.ds(k * self.tall, self.tall), cols]

    def direct(self, dy, k, y):
        ref = self.place(y, self.c, k)
        to = lax.rem(self.y + dy, self.ys) * CORES + self.c
        return pltpu.make_async_remote_copy(
            src_ref=ref, dst_ref=ref, send_sem=self.ds.at[dy - 1, k], recv_sem=self.dr.at[dy - 1, k],
            device_id={"tp": to}, device_id_type=MESH,
        )

    def partner(self, dy, k, c):
        ref = self.place(lax.rem(self.y - dy + self.ys, self.ys), c, k)
        return pltpu.make_async_remote_copy(
            src_ref=ref, dst_ref=ref, send_sem=self.ps.at[dy, k], recv_sem=self.pr.at[dy, k],
            device_id={"tp": self.y * CORES + 1 - self.c}, device_id_type=MESH,
        )

    def go(self, copy):
        copy.start()
        self.sent.append(copy)

    def start(self, k):
        for dy in range(1, self.ys):
            self.go(self.direct(dy, k, self.y))
        self.go(self.partner(0, k, self.c))

    def relay(self, k):
        for dy in range(1, self.ys):
            self.direct(dy, k, lax.rem(self.y - dy + self.ys, self.ys)).wait_recv()
            self.go(self.partner(dy, k, self.c))

    def finish(self, k):
        for dy in range(self.ys):
            self.partner(dy, k, 1 - self.c).wait_recv()

    def drain(self):
        for copy in self.sent:
            copy.wait_send()


def step_kernel(
    n, m, cap,
    q_hbm, f_hbm, v_hbm, g_hbm, floor_ref, hgain_ref, proj_hbm, tok_ref, egain_ref,
    routes_ref, glog_ref, clog_ref, wg_hbm, wu_hbm, wd_hbm,
    mix_out, exp_out,
    q_ref, f_ref, v_ref, g_ref, proj_ref, wg_ref, wu_ref, wd_ref,
    pick0, pick1, slots, xbuf, hbuf, ybuf, rbuf, mbuf, qs_ref, oi_ref,
    s_send, s_recv, d_send, d_recv,
    local_sem, x_s, x_r, r_s, r_r, st_s, st_r,
    xg0, xg1, xg2, xg3, hg0, hg1, hg2, hg3, mg0, mg1, mg2, mg3,
):
    me = lax.axis_index("ep")
    t = lax.axis_index("tp")
    ys = m // CORES
    tokens, width = tok_ref.shape
    wx = width // m
    length, wk = q_ref.shape
    heads = wk // KEYDIM
    wf = wg_ref.shape[1]
    wo = wd_ref.shape[1]
    per = n // BATCHES
    rows_b = per * cap

    def at_ep(k):
        return lax.rem(me + k + n, n)

    loads = []
    pairs = (
        (q_hbm, q_ref), (f_hbm, f_ref), (v_hbm, v_ref), (g_hbm, g_ref),
        (wg_hbm.at[0], wg_ref), (wu_hbm.at[0], wu_ref), (wd_hbm.at[0], wd_ref), (proj_hbm, proj_ref),
    )
    for i, (src, dst) in enumerate(pairs):
        copy = pltpu.make_async_copy(src, dst, local_sem.at[i])
        copy.start()
        loads.append(copy)

    barrier = pltpu.get_barrier_semaphore()
    for k in range(1, n):
        pl.semaphore_signal(barrier, inc=1, device_id={"ep": at_ep(k)}, device_id_type=MESH)
    y, c = t // CORES, t % CORES
    for dy in range(1, ys):
        pl.semaphore_signal(
            barrier, inc=1, device_id={"tp": lax.rem(y + dy, ys) * CORES + c}, device_id_type=MESH
        )
    pl.semaphore_signal(barrier, inc=1, device_id={"tp": y * CORES + 1 - c}, device_id_type=MESH)

    gap = routes_ref[...] - me
    rel = jnp.where(gap < 0, gap + n, gap)
    expert = lax.broadcasted_iota(jnp.int32, (n, tokens), 0)
    is0 = (rel[0:1] == expert).astype(f32)
    is1 = (rel[1:2] == expert).astype(f32)
    before = (
        lax.broadcasted_iota(jnp.int32, (tokens, tokens), 0)
        < lax.broadcasted_iota(jnp.int32, (tokens, tokens), 1)
    ).astype(f32).astype(bf16)
    ranks = mm((is0 + is1).astype(bf16), before)
    slot0 = rel[0:1].astype(f32) * cap + jnp.sum(is0 * ranks, axis=0, keepdims=True)
    slot1 = rel[1:2].astype(f32) * cap + jnp.sum(is1 * ranks, axis=0, keepdims=True)
    slot_ids = lax.broadcasted_iota(jnp.int32, (n * cap, tokens), 0).astype(f32)
    one0 = (slot_ids == slot0).astype(f32)
    one1 = (slot_ids == slot1).astype(f32)
    pick0[...] = one0.astype(bf16)
    pick1[...] = one1.astype(bf16)
    full = tok_ref[...].astype(f32)
    scale = lax.rsqrt(jnp.mean(full * full, axis=-1, keepdims=True) + norm_eps)
    own_cols = pl.ds(pl.multiple_of(t * wx, wx), wx)
    normed = (tok_ref[:, own_cols].astype(f32) * scale * egain_ref[:, own_cols]).astype(bf16)
    slots[...] = mm((one0 + one1).astype(bf16), normed).astype(bf16)
    xbuf[0:cap, own_cols] = slots[0:cap, :]

    pl.semaphore_wait(barrier, (n - 1) + (ys - 1) + 1)

    def x_copy(k):
        return pltpu.make_async_remote_copy(
            src_ref=slots.at[pl.ds(k * cap, cap), :], dst_ref=xbuf.at[pl.ds(k * cap, cap), own_cols],
            send_sem=x_s.at[k - 1], recv_sem=x_r.at[k - 1],
            device_id={"ep": at_ep(k)}, device_id_type=MESH,
        )

    for k in range(1, n):
        x_copy(k).start()
    gx = Gather(xbuf, wx, cap, (t, m), (xg0, xg1, xg2, xg3))
    gx.start(0)

    for i in range(3):
        loads[i].wait()
    rates = (1.0 - floor_ref[...]) * sigmoid(-f_ref[...].astype(f32))
    log_forget = jnp.log(1.0 - rates)
    row = lax.broadcasted_iota(jnp.int32, (length, length), 0)
    col = lax.broadcasted_iota(jnp.int32, (length, length), 1)
    causal = row >= col
    upto = causal.astype(f32).astype(bf16)
    high = log_forget.astype(bf16)
    low = (log_forget - high.astype(f32)).astype(bf16)
    cumulative = mm(upto, high) + mm(upto, low)
    last = cumulative[length - 1 : length, :]
    pre = q_ref[...].astype(f32)
    scaled_q = (pre * sigmoid(pre) * jnp.exp(cumulative)).astype(bf16)
    qs_ref[...] = scaled_q
    scaled_k = (rates * jnp.exp(-cumulative)).astype(bf16)
    tail_k = (rates * jnp.exp(last - cumulative)).astype(bf16)
    states = []
    for h in range(heads):
        cols = slice(h * KEYDIM, (h + 1) * KEYDIM)
        values = v_ref[:, cols]
        scores = jnp.where(causal, mm_nt(scaled_q[:, cols], scaled_k[:, cols]), 0.0).astype(bf16)
        oi_ref[:, cols] = mm(scores, values)
        states.append(mm_tn(values, tail_k[:, cols]))
    win_s = jnp.concatenate(states, axis=1) if heads > 1 else states[0]
    win_a = jnp.exp(last)
    pre_s = jnp.zeros_like(win_s)
    pre_a = jnp.ones_like(win_a)

    def state_copies(r):
        to = {"ep": at_ep(1 << r)}
        return (
            pltpu.make_async_remote_copy(
                src_ref=s_send.at[r], dst_ref=s_recv.at[r], send_sem=st_s.at[0, r], recv_sem=st_r.at[0, r],
                device_id=to, device_id_type=MESH,
            ),
            pltpu.make_async_remote_copy(
                src_ref=d_send.at[r], dst_ref=d_recv.at[r], send_sem=st_s.at[1, r], recv_sem=st_r.at[1, r],
                device_id=to, device_id_type=MESH,
            ),
        )

    rounds = (n - 1).bit_length()

    def state_send(r, a, s):
        s_send[r] = s.astype(bf16)
        d_send[r] = jnp.broadcast_to(a, d_send.shape[1:])

        @pl.when(me + (1 << r) < n)
        def _():
            for copy in state_copies(r):
                copy.start()

    def state_take(r, pre_pair, win_pair):
        @pl.when(me >= (1 << r))
        def _():
            for copy in state_copies(r):
                copy.wait_recv()

        @pl.when(me < (1 << r))
        def _():
            s_recv[r] = jnp.zeros(s_recv.shape[1:], bf16)
            d_recv[r] = jnp.ones(d_recv.shape[1:], f32)

        got_s = s_recv[r].astype(f32)
        got_a = d_recv[r, 0:1, :]
        (pa, ps), (wa, ws) = pre_pair, win_pair
        return (pa * got_a, pa * got_s + ps), (wa * got_a, wa * got_s + ws)

    prefix, window = (pre_a, pre_s), (win_a, win_s)
    state_send(0, *window)

    def forward(k):
        x_copy(k).wait_recv()
        gx.start(k)

    for k in range(1, per):
        forward(k)
        gx.relay(k - 1)
    done = 0
    prefix, window = state_take(0, prefix, window)
    done = 1
    if done < rounds:
        state_send(1, *window)
    for k in range(per, n):
        forward(k)
        if k == per:
            gx.relay(k - 1)
    loads[4].wait()
    loads[5].wait()
    gh = Gather(hbuf, wf, rows_b, (t, m), (hg0, hg1, hg2, hg3))
    own_hidden = pl.ds(pl.multiple_of(t * wf, wf), wf)

    def experts_in(b):
        for k in range(b * per, (b + 1) * per):
            gx.finish(k)
        span = slice(b * rows_b, (b + 1) * rows_b)
        x = xbuf[span, :]
        gate = mm(x, wg_ref[...])
        up = mm(x, wu_ref[...])
        hbuf[span, own_hidden] = (gate * sigmoid(gate) * up).astype(bf16)
        gh.start(b)

    for b in range(BATCHES):
        if b > 0:
            for k in range(b * per, (b + 1) * per):
                gx.relay(k)
        experts_in(b)
        if done < rounds:
            prefix, window = state_take(done, prefix, window)
            done += 1
            if done < rounds:
                state_send(done, *window)
    while done < rounds:
        prefix, window = state_take(done, prefix, window)
        done += 1
        if done < rounds:
            state_send(done, *window)

    loads[3].wait()
    entering = prefix[1].astype(bf16)
    gm = Gather(mbuf, wk, length, (t, m), (mg0, mg1, mg2, mg3))
    for h in range(heads):
        cols = slice(h * KEYDIM, (h + 1) * KEYDIM)
        out = oi_ref[:, cols] + mm_nt(qs_ref[:, cols], entering[:, cols])
        gate = g_ref[:, cols].astype(f32)
        out = out * lax.rsqrt(jnp.mean(out * out, axis=-1, keepdims=True) + norm_eps)
        out = out * hgain_ref[...] * (gate * sigmoid(gate))
        place = pl.ds(pl.multiple_of(t * wk + h * KEYDIM, KEYDIM), KEYDIM)
        mbuf[:, place] = out.astype(bf16)
    gm.start(0)

    def r_copy(k):
        span = pl.ds(k * cap, cap)
        return pltpu.make_async_remote_copy(
            src_ref=ybuf.at[span, :], dst_ref=rbuf.at[span, :],
            send_sem=r_s.at[k - 1], recv_sem=r_r.at[k - 1],
            device_id={"ep": at_ep(-k)}, device_id_type=MESH,
        )

    loads[6].wait()
    for b in range(BATCHES):
        gh.relay(b)
        gh.finish(b)
        span = slice(b * rows_b, (b + 1) * rows_b)
        ybuf[span, :] = mm(hbuf[span, :], wd_ref[...]).astype(bf16)
        for k in range(max(1, b * per), (b + 1) * per):
            r_copy(k).start()

    gm.relay(0)
    gm.finish(0)
    loads[7].wait()
    mix_out[...] = mm(mbuf[...], proj_ref[...]).astype(bf16)

    group_exp = jnp.exp(glog_ref[...])
    group_prob = group_exp / jnp.sum(group_exp, axis=0, keepdims=True)
    size = n // GROUPS
    low_id = lax.broadcasted_iota(jnp.int32, (GROUPS, tokens), 0) * size
    routes = routes_ref[...]
    in0 = ((routes[0:1] >= low_id) & (routes[0:1] < low_id + size)).astype(f32)
    in1 = ((routes[1:2] >= low_id) & (routes[1:2] < low_id + size)).astype(f32)
    same = jnp.sum(in0 * in1, axis=0, keepdims=True)
    choice_exp = jnp.exp(clog_ref[...])
    ce0, ce1 = choice_exp[0:1], choice_exp[1:2]
    w0 = jnp.sum(in0 * group_prob, axis=0, keepdims=True) * ce0 / (ce0 + same * ce1)
    w1 = jnp.sum(in1 * group_prob, axis=0, keepdims=True) * ce1 / (ce1 + same * ce0)
    w0 = jnp.transpose(jnp.broadcast_to(w0, (128, tokens)))[:, 0:1]
    w1 = jnp.transpose(jnp.broadcast_to(w1, (128, tokens)))[:, 0:1]

    rbuf[0:cap, :] = ybuf[0:cap, :]
    for k in range(1, n):
        r_copy(k).wait_recv()
    back = rbuf[...]
    exp_out[...] = (w0 * mm_tn(pick0[...], back) + w1 * mm_tn(pick1[...], back)).astype(bf16)

    for k in range(1, n):
        x_copy(k).wait_send()
        r_copy(k).wait_send()
    for r in range(rounds):
        @pl.when(me + (1 << r) < n)
        def _():
            for copy in state_copies(r):
                copy.wait_send()
    gx.drain()
    gh.drain()
    gm.drain()


def per_device(n, m, mq, mf, mv, mg, floor, hgain, proj, tok, egain, routes, glog, clog, wg, wu, wd):
    length, wk = mq.shape
    tokens, width = tok.shape
    wf, wo = wg.shape[2], wd.shape[2]
    cap = 2 * TOPK * tokens // n
    rows = n * cap
    ys = m // CORES
    rounds = (n - 1).bit_length()
    vmem = pl.BlockSpec(memory_space=pltpu.VMEM)
    hbm = pl.BlockSpec(memory_space=pl.ANY)

    def gather_sems(chunks):
        dma = pltpu.SemaphoreType.DMA
        return [dma((ys - 1, chunks)), dma((ys - 1, chunks)), dma((ys, chunks)), dma((ys, chunks))]

    dma = pltpu.SemaphoreType.DMA
    scratch = [
        pltpu.VMEM((length, wk), bf16), pltpu.VMEM((length, wk), bf16),
        pltpu.VMEM((length, wk), bf16), pltpu.VMEM((length, wk), bf16),
        pltpu.VMEM(proj.shape, bf16),
        pltpu.VMEM(wg.shape[1:], bf16), pltpu.VMEM(wu.shape[1:], bf16), pltpu.VMEM(wd.shape[1:], bf16),
        pltpu.VMEM((rows, tokens), bf16), pltpu.VMEM((rows, tokens), bf16),
        pltpu.VMEM((rows, width // m), bf16),
        pltpu.VMEM((rows, width), bf16),
        pltpu.VMEM((rows, wd.shape[1]), bf16),
        pltpu.VMEM((rows, wo), bf16), pltpu.VMEM((rows, wo), bf16),
        pltpu.VMEM((length, proj.shape[0]), bf16),
        pltpu.VMEM((length, wk), bf16), pltpu.VMEM((length, wk), f32),
        pltpu.VMEM((rounds, KEYDIM, wk), bf16), pltpu.VMEM((rounds, KEYDIM, wk), bf16),
        pltpu.VMEM((rounds, 8, wk), f32), pltpu.VMEM((rounds, 8, wk), f32),
        dma((8,)), dma((n - 1,)), dma((n - 1,)), dma((n - 1,)), dma((n - 1,)),
        dma((2, rounds)), dma((2, rounds)),
    ] + gather_sems(n) + gather_sems(BATCHES) + gather_sems(1)
    return pl.pallas_call(
        functools.partial(step_kernel, n, m, cap),
        out_shape=(
            jax.ShapeDtypeStruct((length, proj.shape[1]), bf16),
            jax.ShapeDtypeStruct((tokens, wo), bf16),
        ),
        in_specs=[hbm, hbm, hbm, hbm, vmem, vmem, hbm, vmem, vmem, vmem, vmem, vmem, hbm, hbm, hbm],
        out_specs=(vmem, vmem),
        scratch_shapes=scratch,
        compiler_params=pltpu.CompilerParams(
            collective_id=0, has_side_effects=True, vmem_limit_bytes=60 * 1024 * 1024
        ),
    )(
        mq, mf, mv, mg, floor[None, :], hgain[None, :], proj, tok, egain[None, :],
        routes.T, glog.T, clog.T, wg, wu, wd,
    )


def solution(mesh):
    return jax.shard_map(
        functools.partial(per_device, mesh.shape["ep"], mesh.shape["tp"]),
        mesh=mesh,
        in_specs=(
            P("ep", "tp"), P("ep", "tp"), P("ep", "tp"), P("ep", "tp"), P("tp"), P(), P(None, "tp"),
            P("ep", None), P(), P("ep", None), P("ep", None), P("ep", None),
            P("ep", None, "tp"), P("ep", None, "tp"), P("ep", None, "tp"),
        ),
        out_specs=(P("ep", "tp"), P("ep", "tp")),
        check_vma=False,
    )
```
